32 devices in a mesh: kv: 8 (over z, y), tp: 4 (over x, core).
Axes of the slice: x: 2, y: 2, z: 4, core: 2. Of those that a mesh axis runs over, the one named last changes fastest.
Arguments:
- tokens: bfloat16 [32, 4096], P(None, 'kv'), may hold values from -8 to 8, as said below
- attn_gain: float32 [4096], P('kv'), may hold values from 0.1 to 1.9
- query_weight: bfloat16 [4096, 1024], P('kv', 'tp'), may hold values from -0.09375 to 0.09375
- key_weight: bfloat16 [4096, 1024], P('kv', 'tp'), may hold values from -0.09375 to 0.09375
- value_weight: bfloat16 [4096, 2048], P('kv', 'tp'), may hold values from -0.09375 to 0.09375
- outgate_weight: bfloat16 [4096, 2048], P('kv', 'tp'), may hold values from -0.09375 to 0.09375
- code_weight: bfloat16 [4096, 16], P('kv'), may hold values from -0.09375 to 0.09375
- decay_weight: bfloat16 [16, 1024], P(None, 'tp'), may hold values from -6 to 6
- decay_bias: float32 [1024], P('tp'), may hold values from -4 to 2
- head_gain: float32 [256], replicated, may hold values from 0.1 to 1.9
- key_cache: bfloat16 [32, 64, 8, 128], P('kv', None, 'tp'), may hold values from -6 to 6
- value_cache: bfloat16 [32, 64, 8, 256], P('kv', None, 'tp'), may hold values from -6 to 6
- decay_cache: float32 [32, 64, 8, 128], P('kv', None, 'tp'), may hold values from -1.1 to 0
- carried_state: float32 [32, 8, 128, 256], P('kv', 'tp'), may hold values from -24 to 24
- lengths: int32 [32], P('kv'), may hold values from 1 to 64, 832 in all
- output_weight: bfloat16 [2048, 4096], P('tp', 'kv'), may hold values from -0.125 to 0.125
- mlp_gain: float32 [4096], P('kv'), may hold values from 0.1 to 1.9
- gate_weight: bfloat16 [4096, 11008], P('kv', 'tp'), may hold values from -0.09375 to 0.09375
- up_weight: bfloat16 [4096, 11008], P('kv', 'tp'), may hold values from -0.09375 to 0.09375
- down_weight: bfloat16 [11008, 4096], P('tp', 'kv'), may hold values from -0.0546875 to 0.0546875
Outputs:
- layer_out: bfloat16 [32, 4096], P(None, 'kv')
- new_keys: bfloat16 [32, 8, 128], P('kv', 'tp')
- new_values: bfloat16 [32, 8, 256], P('kv', 'tp')
The draws below stay inside these ranges and needn't reach their ends.
Inputs may be any that keep to these rules, and one draw needn't show every extreme that they name: `tokens`: the features of a row have unlike scales. Sequence b's new token comes right after its lengths[b] live positions; positions from lengths[b] on take no part.
All inputs are finite; a program needn't handle non-finite values. No bound on the sum of `lengths` on one device may be relied on, other than what follows from the above.
Results may differ from the reference program's by a relative error of at most 0.025.
Values may be sent and summed in bfloat16 or wider, within the bound.
A program may use at most 64 MiB of HBM per device.

```python
import math
import jax
import jax.numpy as jnp
import numpy as np
from jax import lax

WIDTH = 4096
HEAD_COUNT = 8
KEY_DIM = 128
VALUE_DIM = 256
KEY_WIDTH = 1024
VALUE_WIDTH = 2048
GATE_RANK = 16
MLP_WIDTH = 11008
BLOCK_SPAN = 64
BATCH_TOTAL = 32
N_TP = 4


def draw_tokens(key, part):
    base_key, rough_key = jax.random.split(jax.random.fold_in(key, 11), 2)
    column = jnp.arange(WIDTH, dtype=jnp.float32) / WIDTH
    jaggedness = jax.random.uniform(rough_key, (WIDTH,), jnp.float32, 0.5, 2.0)
    scales = 10.0 ** (column - 0.75) * jaggedness
    values = jax.random.normal(base_key, (BATCH_TOTAL, WIDTH), jnp.float32) * scales[None, :]
    return jnp.clip(values, -8.0, 8.0).astype(jnp.bfloat16)


def draw_decay_cache(key, part):
    random_split_keys = jax.random.split(jax.random.fold_in(key, 23), 5)
    slowest = 0.002
    fastest = 0.12
    channel_frequencies = jnp.exp(jax.random.uniform(random_split_keys[0], (1, 1, HEAD_COUNT, KEY_DIM), jnp.float32, math.log(slowest), math.log(fastest)))
    sequence_wise = jnp.exp(jax.random.uniform(random_split_keys[1], (BATCH_TOTAL, 1, 1, 1), jnp.float32, math.log(0.5), math.log(2.0)))
    jaggedness = jax.random.uniform(random_split_keys[2], (BATCH_TOTAL, BLOCK_SPAN, HEAD_COUNT, KEY_DIM), jnp.float32, 0.5, 1.5)
    spike_events = jax.random.randint(random_split_keys[3], (BATCH_TOTAL, BLOCK_SPAN, 1, 1), 0, BLOCK_SPAN) < 3
    spike_removal = jax.random.uniform(random_split_keys[4], (BATCH_TOTAL, BLOCK_SPAN, HEAD_COUNT, 1), jnp.float32, math.log(0.5), math.log(0.8))
    return -channel_frequencies * sequence_wise * jaggedness + jnp.where(spike_events, spike_removal, 0.0)


def levels(stream_key, extent, shards, smallest, top_value):
    def one(dim, blocks):
        heights = jax.random.uniform(jax.random.fold_in(jax.random.fold_in(stream_key, 6), dim), (blocks,), jnp.float32, smallest / len(shards), top_value / len(shards))
        return jnp.repeat(jnp.exp(heights), extent[dim] // blocks).reshape((-1,) + (1,) * (len(extent) - dim - 1))

    level = one(*shards[0])
    for cut in shards[1:]:
        level = level * one(*cut)
    return level


def split_up(amount, total, limit, slope):
    loads = [(1 << 20) // math.isqrt(grade ** slope) + 1 for grade in range(2, amount + 1)]
    surplus, given = total - limit - (amount - 1), [1] * (amount - 1)
    while surplus > 0:
        candidates = [i for i in range(amount - 1) if given[i] < limit]
        whole, remaining = sum([loads[i] for i in candidates]), surplus
        for i in candidates:
            more = min(limit - given[i], max(1, remaining * loads[i] // whole), surplus)
            given[i] = given[i] + more
            surplus = surplus - more
    return np.array([limit] + given)


def ragged_sizes(own_key, count, total, limit, slope):
    if count == 2:
        one = jax.random.randint(own_key, (), max(1, total - limit), min(limit, total - 1) + 1)
        return jnp.stack([one, total - one])
    sizes = jnp.asarray(split_up(count, total, limit, slope), jnp.int32)
    couples = (count - 1) // 2
    source_of, taker = sizes[1:1 + 2 * couples:2], sizes[2:2 + 2 * couples:2]
    room = jnp.minimum(source_of - 1, limit - taker)
    shifted = jax.random.randint(jax.random.fold_in(own_key, 1), (couples,), 0, 1 << 20) % (room + 1)
    sizes = sizes.at[1:1 + 2 * couples:2].set(source_of - shifted).at[2:2 + 2 * couples:2].set(taker + shifted)
    return sizes[jax.random.permutation(jax.random.fold_in(own_key, 2), count)]


def scatter_about(own_key, dims, scale, most, pieces=(), kind=jnp.bfloat16):
    result = jax.random.normal(own_key, dims, jnp.float32) * scale
    if len(pieces) > 0:
        result = levels(own_key, dims, pieces, -0.22, 0.18) * result
    return jnp.clip(result, min=-most, max=most).astype(kind)


def setup_inputs(seed: int = 0) -> dict:
    streams_of = jax.random.split(jax.random.key(seed), 21)
    return {
        "tokens": draw_tokens(jax.random.fold_in(streams_of[20], 71), 0),
        "attn_gain": jnp.clip(1.0 + 0.18 * jax.random.normal(streams_of[1], (WIDTH,), jnp.float32), 0.1, 1.9),
        "query_weight": scatter_about(streams_of[2], (WIDTH, KEY_WIDTH), WIDTH ** -0.5, 0.09375, ((0, 8), (1, 4))),
        "key_weight": scatter_about(streams_of[3], (WIDTH, KEY_WIDTH), WIDTH ** -0.5, 0.09375, ((0, 8), (1, 4))),
        "value_weight": scatter_about(streams_of[4], (WIDTH, VALUE_WIDTH), WIDTH ** -0.5, 0.09375, ((0, 8), (1, 4))),
        "outgate_weight": scatter_about(streams_of[5], (WIDTH, VALUE_WIDTH), WIDTH ** -0.5, 0.09375, ((0, 8), (1, 4))),
        "code_weight": scatter_about(streams_of[6], (WIDTH, GATE_RANK), WIDTH ** -0.5, 0.09375, ((0, 8),)),
        "decay_weight": scatter_about(streams_of[7], (GATE_RANK, KEY_WIDTH), 1 ** -0.5, 6.0, ((1, 4),)),
        "decay_bias": jnp.clip(-4.0 + 6.0 * jax.random.uniform(streams_of[8], (KEY_WIDTH,), jnp.float32) ** levels(streams_of[8], (KEY_WIDTH,), ((0, 4),), -0.2, 0.2), -4.0, 2.0),
        "head_gain": jnp.clip(1.0 + 0.18 * jax.random.normal(streams_of[9], (VALUE_DIM,), jnp.float32), 0.1, 1.9),
        "key_cache": scatter_about(streams_of[10], (BATCH_TOTAL, BLOCK_SPAN, HEAD_COUNT, KEY_DIM), 1.0, 6.0, ((0, 8), (2, 4))),
        "value_cache": scatter_about(streams_of[11], (BATCH_TOTAL, BLOCK_SPAN, HEAD_COUNT, VALUE_DIM), 1.0, 6.0, ((0, 8), (2, 4))),
        "decay_cache": draw_decay_cache(jax.random.fold_in(streams_of[20], 71), 0),
        "carried_state": scatter_about(streams_of[13], (BATCH_TOTAL, HEAD_COUNT, KEY_DIM, VALUE_DIM), 4.0, 24.0, ((0, 8), (1, 4)), jnp.float32),
        "lengths": ragged_sizes(streams_of[14], BATCH_TOTAL, BATCH_TOTAL * (13 * BLOCK_SPAN // 32), BLOCK_SPAN, 2).astype(jnp.int32),
        "output_weight": scatter_about(streams_of[15], (VALUE_WIDTH, WIDTH), VALUE_WIDTH ** -0.5, 0.125, ((0, 4), (1, 8))),
        "mlp_gain": jnp.clip(1.0 + 0.18 * jax.random.normal(streams_of[16], (WIDTH,), jnp.float32), 0.1, 1.9),
        "gate_weight": scatter_about(streams_of[17], (WIDTH, MLP_WIDTH), WIDTH ** -0.5, 0.09375, ((0, 8), (1, 4))),
        "up_weight": scatter_about(streams_of[18], (WIDTH, MLP_WIDTH), WIDTH ** -0.5, 0.09375, ((0, 8), (1, 4))),
        "down_weight": scatter_about(streams_of[19], (MLP_WIDTH, WIDTH), MLP_WIDTH ** -0.5, 0.0546875, ((0, 4), (1, 8))),
    }


EPS = 1e-06
GATE_TEMP = 16.0

def block_attention(queries, new_keys, new_values, new_decay, key_cache, value_cache, decay_cache, carried_state, lengths):
    positions = jnp.arange(key_cache.shape[1], dtype=jnp.int32)
    live_mask = positions[None, :] < lengths[:, None]
    kept_decay = jnp.where(live_mask[:, :, None, None], decay_cache, jnp.zeros_like(decay_cache))
    later_sum = lax.cumsum(kept_decay, axis=1, reverse=True) - kept_decay
    total_decay = lax.optimization_barrier(jnp.sum(kept_decay, axis=1))
    decayed = queries.astype(jnp.float32) * jnp.exp(new_decay)
    carried = jnp.einsum('bhd,bhde->bhe', decayed * jnp.exp(total_decay), carried_state, precision=lax.Precision.HIGHEST)
    keyed_cache = key_cache.astype(jnp.float32) * jnp.exp(later_sum)
    scores = jnp.einsum('bhd,bshd->bhs', decayed, keyed_cache, precision=lax.Precision.HIGHEST)
    scores = jnp.where(live_mask[:, None, :], scores, jnp.zeros_like(scores)).astype(jnp.bfloat16)
    within = jnp.einsum('bhs,bshe->bhe', scores.astype(jnp.float32), value_cache.astype(jnp.float32))
    own_score = lax.optimization_barrier(jnp.sum(queries.astype(jnp.float32) * new_keys.astype(jnp.float32), axis=-1))
    return carried + within + own_score[..., None] * new_values.astype(jnp.float32)

def summed_by_group(left, weight, groups):
    row_count, inner_dim = left.shape
    group_parts = jnp.einsum('bni,nid->bnd', left.reshape(row_count, groups, inner_dim // groups).astype(jnp.float32), weight.reshape(groups, inner_dim // groups, weight.shape[1]).astype(jnp.float32))
    group_parts = lax.optimization_barrier(group_parts.astype(jnp.bfloat16))
    return lax.optimization_barrier(jnp.sum(group_parts.astype(jnp.float32), axis=1))

def reference(tokens, attn_gain, query_weight, key_weight, value_weight, outgate_weight, code_weight, decay_weight, decay_bias, head_gain, key_cache, value_cache, decay_cache, carried_state, lengths, output_weight, mlp_gain, gate_weight, up_weight, down_weight):
    token_f = tokens.astype(jnp.float32)
    scaled = (token_f * attn_gain[None, :]).astype(jnp.bfloat16)
    inv_rms = lax.rsqrt(lax.optimization_barrier(jnp.mean(token_f * token_f, axis=1, keepdims=True)) + EPS)

    def project(weight):
        return jnp.dot(scaled, weight, preferred_element_type=jnp.float32) * inv_rms
    queries = (project(query_weight) * KEY_DIM ** (-0.5)).astype(jnp.bfloat16).reshape(BATCH_TOTAL, HEAD_COUNT, KEY_DIM)
    new_keys = project(key_weight).astype(jnp.bfloat16).reshape(BATCH_TOTAL, HEAD_COUNT, KEY_DIM)
    new_values = project(value_weight).astype(jnp.bfloat16).reshape(BATCH_TOTAL, HEAD_COUNT, VALUE_DIM)
    out_gate = project(outgate_weight).astype(jnp.bfloat16).reshape(BATCH_TOTAL, HEAD_COUNT, VALUE_DIM)
    gate_code = project(code_weight).astype(jnp.bfloat16)
    pre_gate = jnp.dot(gate_code, decay_weight, preferred_element_type=jnp.float32) + decay_bias[None, :]
    new_decay = (jax.nn.log_sigmoid(pre_gate) / GATE_TEMP).reshape(BATCH_TOTAL, HEAD_COUNT, KEY_DIM)
    mixed_heads = block_attention(queries, new_keys, new_values, new_decay, key_cache, value_cache, decay_cache, carried_state, lengths)
    normed = mixed_heads * lax.rsqrt(lax.optimization_barrier(jnp.mean(mixed_heads * mixed_heads, axis=-1, keepdims=True)) + EPS) * head_gain
    heads_out = (normed * jax.nn.silu(out_gate.astype(jnp.float32))).astype(jnp.bfloat16).reshape(BATCH_TOTAL, HEAD_COUNT * VALUE_DIM)
    attended = summed_by_group(heads_out, output_weight, N_TP)
    middle = (token_f + attended).astype(jnp.bfloat16)
    mid_f = middle.astype(jnp.float32)
    scaled_mid = (mid_f * mlp_gain[None, :]).astype(jnp.bfloat16)
    inv_mid = lax.rsqrt(lax.optimization_barrier(jnp.mean(mid_f * mid_f, axis=1, keepdims=True)) + EPS)
    gate_act = jnp.dot(scaled_mid, gate_weight, preferred_element_type=jnp.float32) * inv_mid
    up_act = jnp.dot(scaled_mid, up_weight, preferred_element_type=jnp.float32) * inv_mid
    hidden = (jax.nn.silu(gate_act) * up_act).astype(jnp.bfloat16)
    lifted = summed_by_group(hidden, down_weight, N_TP)
    layer_out = (mid_f + lifted).astype(jnp.bfloat16)
    return (layer_out, new_keys, new_values)
```

```python
import functools

import jax
import jax.numpy as jnp
from jax import lax
from jax.experimental import pallas as pl
from jax.experimental.pallas import tpu as pltpu
from jax.sharding import PartitionSpec as P

EPS = 1e-06
GATE_TEMP = 16.0
FIRST_LOADS = 7
PARTS = 4
SHARED_SEMS = 5
LANES = 128
F32 = jnp.float32
BF16 = jnp.bfloat16


def split_sum(column):
    high = column.astype(BF16).astype(F32)
    return high, column - high


def dot(left, right):
    return jnp.dot(left, right, preferred_element_type=F32)


def dot_t(left, right):
    return lax.dot_general(left, right, (((1,), (1,)), ((), ())), preferred_element_type=F32)


def tiles_of(total, step):
    return [(start, min(step, total - start)) for start in range(0, total, step)]


def pieces_of(units):
    each = units // PARTS // LANES * LANES
    head = units - (PARTS - 1) * each
    room = (head + 2 + LANES - 1) // LANES * LANES
    return [(0, head, room)] + [(head + k * each, each, each) for k in range(PARTS - 1)]


def peer_of(me, step, count):
    if count & (count - 1):
        return lax.rem(me + step, count)
    place, bit = 0, 1
    while bit < count:
        own = lax.rem(me // bit, 2)
        place = place + bit * (1 - own if step & bit else own)
        bit *= 2
    return place


def drain(ref, sem):
    pltpu.make_async_copy(ref, ref, sem).wait()


def copy_out(*refs):
    *arrays, sems = refs
    half = len(arrays) // 2
    copies = [
        pltpu.make_async_copy(arrays[k], arrays[half + k], sems.at[k]) for k in range(half)
    ]
    for copy in copies:
        copy.start()
    for copy in copies:
        copy.wait()


def layer_kernel(
    n_kv,
    n_tp,
    width,
    tokens_h,
    attn_gain_h,
    wq_h,
    wk_h,
    wv_h,
    wg_h,
    wc_h,
    dw_h,
    db_h,
    head_gain_h,
    key_h,
    value_h,
    decay_h,
    state_h,
    lengths_h,
    wo_h,
    mlp_gain_h,
    gate_h,
    up_h,
    down_h,
    out_ref,
    nk_ref,
    nv_ref,
    tokens,
    attn_gain,
    wq,
    wk,
    wv,
    wg,
    wc,
    dw,
    db,
    head_gain,
    key,
    value,
    decay,
    state,
    lengths_s,
    wo,
    mlp_gain,
    gate,
    up,
    down,
    early,
    early_send,
    early_recv,
    proj,
    proj_send,
    proj_recv,
    keyed,
    total_exp,
    decayed3,
    keys3,
    values3,
    mixed,
    heads,
    heads_all,
    attended,
    accs,
    sends,
    recvs,
    hiddens,
    hiddens_all,
    lifted,
    load_sem,
    send_sem,
    recv_sem,
):
    kv_me = lax.axis_index("kv")
    tp_me = lax.axis_index("tp")
    rows, feats = tokens.shape
    seqs, span, heads_here, key_dim = key.shape
    value_dim = value.shape[3]
    kw, vw = heads_here * key_dim, heads_here * value_dim
    rank = wc.shape[0]
    units = gate.shape[0]
    pieces = pieces_of(units)

    loads = {}
    pairs = [
        ("tokens", tokens_h, tokens),
        ("attn_gain", attn_gain_h, attn_gain),
        ("wc", wc_h, wc),
        ("wq", wq_h, wq),
        ("wk", wk_h, wk),
        ("wv", wv_h, wv),
        ("wg", wg_h, wg),
        ("lengths", lengths_h, lengths_s),
        ("decay", decay_h, decay),
        ("key", key_h, key),
        ("dw", dw_h, dw.at[pl.ds(0, rank)]),
        ("db", db_h, db),
        ("head_gain", head_gain_h, head_gain),
        ("state", state_h, state),
        ("value", value_h, value),
        ("wo", wo_h, wo),
        ("mlp_gain", mlp_gain_h, mlp_gain),
        ("gate", gate_h, gate),
        ("up", up_h, up),
        ("down", down_h, down),
    ]
    for place, (name, source, target) in enumerate(pairs):
        loads[name] = pltpu.make_async_copy(source, target, load_sem.at[place])
        if place < FIRST_LOADS:
            loads[name].start()

    def ready(*names):
        for name in names:
            loads.pop(name).wait()

    barrier = pltpu.get_barrier_semaphore()
    for off in range(1, n_kv):
        pl.semaphore_signal(
            barrier,
            inc=1,
            device_id={"kv": lax.rem(kv_me + off, n_kv)},
            device_id_type=pl.DeviceIdType.MESH,
        )
    for off in range(1, n_tp):
        pl.semaphore_signal(
            barrier,
            inc=1,
            device_id={"tp": lax.rem(tp_me + off, n_tp)},
            device_id_type=pl.DeviceIdType.MESH,
        )

    pending = []

    def exchange(axis, me, count, source, target, sem):
        for step in range(count - 1, 0, -1):
            p = peer_of(me, step, count)
            pltpu.make_async_remote_copy(
                src_ref=source(p),
                dst_ref=target.at[me],
                send_sem=send_sem.at[sem],
                recv_sem=recv_sem.at[sem],
                device_id={axis: p},
                device_id_type=pl.DeviceIdType.MESH,
            ).start()
        pending.append((target.at[pl.ds(0, count - 1)], sem))

    def await_arrivals(count, target, sem):
        drain(target.at[pl.ds(0, count - 1)], recv_sem.at[sem])

    base_misc = 2 * kw
    ready(*("tokens", "attn_gain", "wc"))
    token_f = tokens[...].astype(F32)
    scaled = (token_f * attn_gain[...]).astype(BF16)
    early[:, base_misc:] = jnp.zeros((rows, LANES), F32)
    early[:, base_misc : base_misc + rank] = dot_t(scaled, wc[...])
    high, low = split_sum(jnp.sum(token_f * token_f, axis=1, keepdims=True))
    early[:, base_misc + rank : base_misc + rank + 1] = high
    early[:, base_misc + rank + 1 : base_misc + rank + 2] = low

    def project(result, base, name, weight):
        ready(name)
        if name == "wg":
            for late in list(loads.values()):
                late.start()
        for start, size in tiles_of(weight.shape[1], 256):
            result[:, base + start : base + start + size] = dot(
                scaled, weight[:, start : start + size]
            )

    def scatter(result, outgoing, incoming, sem):
        for p in range(n_kv):
            outgoing[p] = result[p * seqs : (p + 1) * seqs, :].astype(BF16)
        exchange("kv", kv_me, n_kv, lambda p: outgoing.at[p], incoming, sem)
        incoming[kv_me] = outgoing[kv_me]

    project(early, 0, "wq", wq)
    project(early, kw, "wk", wk)
    pl.semaphore_wait(barrier, n_kv + n_tp - 2)
    scatter(early, early_send, early_recv, 0)
    project(proj, 0, "wv", wv)
    project(proj, vw, "wg", wg)
    scatter(proj, proj_send, proj_recv, 1)

    dw[rank:, :] = jnp.zeros((dw.shape[0] - rank, dw.shape[1]), BF16)
    ready(*("lengths", "decay", "key"))
    positions = lax.broadcasted_iota(jnp.int32, (span, heads_here, key_dim), 0)
    for b in range(seqs):
        live = positions < lengths_s[b]
        kept = jnp.where(live, decay[b], 0.0)
        suffix = kept
        step = 1
        while step < span:
            suffix = suffix + jnp.concatenate(
                [suffix[step:], jnp.zeros((step, heads_here, key_dim), F32)], axis=0
            )
            step *= 2
        total_exp[b] = jnp.exp(suffix[0])
        later = jnp.concatenate([suffix[1:], jnp.zeros((1, heads_here, key_dim), F32)], axis=0)
        keyed[b] = jnp.where(live, key[b].astype(F32) * jnp.exp(later), 0.0)
    ready(*("dw", "db", "head_gain", "state", "value"))

    def gathered(incoming):
        total = incoming[0].astype(F32)
        for p in range(1, n_kv):
            total = total + incoming[p].astype(F32)
        return total

    await_arrivals(n_kv, early_recv, 0)
    total = gathered(early_recv)
    misc = total[:, base_misc:]
    squares = misc[:, rank : rank + 1] + misc[:, rank + 1 : rank + 2]
    inv_rms = lax.rsqrt(squares / width + EPS)
    queries = (total[:, :kw] * inv_rms * key_dim ** (-0.5)).astype(BF16).astype(F32)
    new_keys = (total[:, kw : 2 * kw] * inv_rms).astype(BF16).astype(F32)
    code = (misc * inv_rms).astype(BF16)
    pre_gate = dot(code, dw[...]) + db[...]
    new_decay = (jnp.minimum(pre_gate, 0.0) - jnp.log1p(jnp.exp(-jnp.abs(pre_gate)))) / GATE_TEMP
    decayed = queries * jnp.exp(new_decay)
    for b in range(seqs):
        for h in range(heads_here):
            k_cols = slice(h * key_dim, (h + 1) * key_dim)
            decayed3[b, h : h + 1, :] = decayed[b : b + 1, k_cols]
            keys3[b, h : h + 1, :] = new_keys[b : b + 1, k_cols]
    nk_ref[...] = keys3[...].astype(BF16)
    for b in range(seqs):
        d = decayed3[b]
        scores = jnp.sum(keyed[b] * d[None], axis=-1, keepdims=True)
        scores = scores.astype(BF16).astype(F32)
        within = jnp.sum(scores * value[b].astype(F32), axis=0)
        into_state = jnp.transpose(
            jnp.concatenate(
                [d * total_exp[b], jnp.zeros((8 - heads_here, key_dim), F32)], axis=0
            )
        )
        for h in range(heads_here):
            carried = jnp.sum(into_state[:, h : h + 1] * state[b, h], axis=0, keepdims=True)
            mixed[b : b + 1, h * value_dim : (h + 1) * value_dim] = carried + within[h : h + 1]
    await_arrivals(n_kv, proj_recv, 1)
    total = gathered(proj_recv)
    new_values = (total[:, :vw] * inv_rms).astype(BF16).astype(F32)
    out_gate = (total[:, vw:] * inv_rms).astype(BF16).astype(F32)
    for h in range(heads_here):
        k_cols = slice(h * key_dim, (h + 1) * key_dim)
        v_cols = slice(h * value_dim, (h + 1) * value_dim)
        own = jnp.sum(queries[:, k_cols] * new_keys[:, k_cols], axis=-1, keepdims=True)
        full = mixed[:, v_cols] + own * new_values[:, v_cols]
        norm = lax.rsqrt(jnp.mean(full * full, axis=-1, keepdims=True) + EPS)
        g = out_gate[:, v_cols]
        mixed[:, v_cols] = full * norm * head_gain[...] * (g / (1.0 + jnp.exp(-g)))
    heads_all[kv_me] = mixed[...].astype(BF16)
    exchange("kv", kv_me, n_kv, lambda p: heads_all.at[kv_me], heads_all, 2)
    for b in range(seqs):
        for h in range(heads_here):
            v_cols = slice(h * value_dim, (h + 1) * value_dim)
            values3[b, h : h + 1, :] = new_values[b : b + 1, v_cols]
    nv_ref[...] = values3[...].astype(BF16)

    ready("wo")
    ready("mlp_gain")
    await_arrivals(n_kv, heads_all, 2)
    for p in range(n_kv):
        heads[p * seqs : (p + 1) * seqs, :] = heads_all[p].astype(F32)
    attended[tp_me] = dot(heads[...].astype(BF16), wo[...]).astype(BF16)
    exchange("tp", tp_me, n_tp, lambda p: attended.at[tp_me], attended, 3)
    ready("gate")
    await_arrivals(n_tp, attended, 3)
    summed = attended[0].astype(F32)
    for p in range(1, n_tp):
        summed = summed + attended[p].astype(F32)
    mid_f = (token_f + summed).astype(BF16).astype(F32)
    scaled_mid = (mid_f * mlp_gain[...]).astype(BF16)

    ready("up")
    for part, (first, size, span_cols) in enumerate(pieces):
        mlp_acc = accs[part]
        for base, weight in ((0, gate), (span_cols, up)):
            if size < span_cols:
                mlp_acc[:, base + span_cols - LANES : base + span_cols] = jnp.zeros(
                    (rows, LANES), F32
                )
            for start, count in tiles_of(size, 256):
                mlp_acc[:, base + start : base + start + count] = dot_t(
                    scaled_mid, weight[first + start : first + start + count, :]
                )
        if part == 0:
            high, low = split_sum(jnp.sum(mid_f * mid_f, axis=1, keepdims=True))
            mlp_acc[:, size : size + 1] = high
            mlp_acc[:, size + 1 : size + 2] = low
        for p in range(n_kv):
            sends[part][p] = mlp_acc[p * seqs : (p + 1) * seqs, :].astype(BF16)
        exchange(
            "kv",
            kv_me,
            n_kv,
            lambda p, part=part: sends[part].at[p],
            recvs[part],
            SHARED_SEMS + part,
        )
        recvs[part][kv_me] = sends[part][kv_me]
    for part, (first, size, span_cols) in enumerate(pieces):
        await_arrivals(n_kv, recvs[part], SHARED_SEMS + part)
        total = gathered(recvs[part])
        if part == 0:
            squares = total[:, size : size + 1] + total[:, size + 1 : size + 2]
            inv_mid = lax.rsqrt(squares / width + EPS)
        g = total[:, :span_cols] * inv_mid
        mine = g / (1.0 + jnp.exp(-g)) * (total[:, span_cols:] * inv_mid)
        hiddens_all[part][kv_me] = mine.astype(BF16)
        exchange(
            "kv",
            kv_me,
            n_kv,
            lambda p, part=part: hiddens_all[part].at[kv_me],
            hiddens_all[part],
            SHARED_SEMS + PARTS + part,
        )
    ready("down")
    acc = jnp.zeros((rows, feats), F32)
    for part, (first, size, span_cols) in enumerate(pieces):
        await_arrivals(n_kv, hiddens_all[part], SHARED_SEMS + PARTS + part)
        hidden = hiddens[part]
        for p in range(n_kv):
            hidden[p * seqs : (p + 1) * seqs, :] = hiddens_all[part][p].astype(F32)
        if size < span_cols:
            lane = lax.broadcasted_iota(jnp.int32, (rows, span_cols), 1)
            whole = jnp.where(lane < size, hidden[...], 0.0).astype(BF16)
        else:
            whole = hidden[...].astype(BF16)
        acc = acc + dot(whole, down[first : first + span_cols, :])
    lifted[tp_me] = acc.astype(BF16)
    exchange("tp", tp_me, n_tp, lambda p: lifted.at[tp_me], lifted, 4)
    await_arrivals(n_tp, lifted, 4)
    summed = lifted[0].astype(F32)
    for p in range(1, n_tp):
        summed = summed + lifted[p].astype(F32)
    out_ref[...] = (mid_f + summed).astype(BF16)
    for ref, sem in pending:
        drain(ref, send_sem.at[sem])


def on_device(n_kv, n_tp, *args):
    (
        tokens,
        attn_gain,
        wq,
        wk,
        wv,
        wg,
        wc,
        dw,
        db,
        head_gain,
        key,
        value,
        decay,
        state,
        lengths,
        wo,
        mlp_gain,
        gate,
        up,
        down,
    ) = args
    row = lambda a: a.reshape(1, a.shape[0])
    operands = [
        tokens,
        row(attn_gain),
        wq,
        wk,
        wv,
        wg,
        wc.T,
        dw,
        row(db),
        row(head_gain),
        key,
        value,
        decay,
        state,
        lengths,
        wo,
        row(mlp_gain),
        gate.T,
        up.T,
        down,
    ]
    rows, feats = tokens.shape
    seqs, span, heads_here, key_dim = key.shape
    value_dim = value.shape[3]
    kw, vw = heads_here * key_dim, heads_here * value_dim
    units = gate.shape[1]
    rank = wc.shape[1]
    widths = [piece[2] for piece in pieces_of(units)]
    first_cols = 2 * kw + LANES
    cols = 2 * vw
    vmem = pltpu.VMEM

    def copied(a):
        if a is lengths:
            return pltpu.SMEM(a.shape, a.dtype)
        if a is dw:
            return vmem((LANES, a.shape[1]), a.dtype)
        return vmem(a.shape, a.dtype)

    scratch = [copied(a) for a in operands]
    scratch += [
        vmem((rows, first_cols), F32),
        vmem((n_kv, seqs, first_cols), BF16),
        vmem((n_kv, seqs, first_cols), BF16),
        vmem((rows, cols), F32),
        vmem((n_kv, seqs, cols), BF16),
        vmem((n_kv, seqs, cols), BF16),
        vmem((seqs, span, heads_here, key_dim), F32),
        vmem((seqs, heads_here, key_dim), F32),
        vmem((seqs, heads_here, key_dim), F32),
        vmem((seqs, heads_here, key_dim), F32),
        vmem((seqs, heads_here, value_dim), F32),
        vmem((seqs, vw), F32),
        vmem((rows, vw), F32),
        vmem((n_kv, seqs, vw), BF16),
        vmem((n_tp, rows, feats), BF16),
        [vmem((rows, 2 * w), F32) for w in widths],
        [vmem((n_kv, seqs, 2 * w), BF16) for w in widths],
        [vmem((n_kv, seqs, 2 * w), BF16) for w in widths],
        [vmem((rows, w), F32) for w in widths],
        [vmem((n_kv, seqs, w), BF16) for w in widths],
        vmem((n_tp, rows, feats), BF16),
    ]
    dma = pltpu.SemaphoreType.DMA
    scratch += [dma((len(operands),))]
    scratch += [dma((SHARED_SEMS + 2 * PARTS,))] * 2
    in_specs = [pl.BlockSpec(memory_space=pltpu.HBM)] * len(operands)
    shapes = ((rows, feats), (seqs, heads_here, key_dim), (seqs, heads_here, value_dim))
    results = pl.pallas_call(
        functools.partial(layer_kernel, n_kv, n_tp, feats * n_kv),
        out_shape=tuple(vmem(shape, BF16) for shape in shapes),
        in_specs=in_specs,
        out_specs=(pl.BlockSpec(memory_space=pltpu.VMEM),) * 3,
        scratch_shapes=scratch,
        compiler_params=pltpu.CompilerParams(
            collective_id=0, has_side_effects=True, vmem_limit_bytes=66900000
        ),
        name="layer",
    )(*operands)
    return pl.pallas_call(
        copy_out,
        out_shape=tuple(jax.ShapeDtypeStruct(shape, BF16) for shape in shapes),
        in_specs=(pl.BlockSpec(memory_space=pltpu.VMEM),) * 3,
        out_specs=(pl.BlockSpec(memory_space=pl.ANY),) * 3,
        scratch_shapes=[dma((3,))],
        name="results",
    )(*results)


def solution(mesh):
    in_specs = (
        P(None, "kv"),
        P("kv"),
        P("kv", "tp"),
        P("kv", "tp"),
        P("kv", "tp"),
        P("kv", "tp"),
        P("kv", None),
        P(None, "tp"),
        P("tp"),
        P(),
        P("kv", None, "tp", None),
        P("kv", None, "tp", None),
        P("kv", None, "tp", None),
        P("kv", "tp", None, None),
        P("kv"),
        P("tp", "kv"),
        P("kv"),
        P("kv", "tp"),
        P("kv", "tp"),
        P("tp", "kv"),
    )
    out_specs = (P(None, "kv"), P("kv", "tp", None), P("kv", "tp", None))
    return jax.shard_map(
        functools.partial(on_device, mesh.shape["kv"], mesh.shape["tp"]),
        mesh=mesh,
        in_specs=in_specs,
        out_specs=out_specs,
        check_vma=False,
    )
```

```python
import functools

import jax
import jax.numpy as jnp
from jax import lax
from jax.experimental import pallas as pl
from jax.experimental.pallas import tpu as pltpu
from jax.sharding import PartitionSpec as P

EPS = 1e-06
GATE_TEMP = 16.0
FIRST_LOADS = 7
SHARES = (4, 6, 7, 5)
PARTS = len(SHARES)
LANES = 128
SWAPPED_LOADS = ("decay", "key", "dw", "db", "state", "value")
SEM_EARLY, SEM_PROJ, SEM_HEADS, SEM_ATTEND, SEM_LIFT, SEM_KEYS, SEM_VALUES = range(7)
SHARED_SEMS = 7
F32 = jnp.float32
BF16 = jnp.bfloat16


def split_sum(column):
    high = column.astype(BF16).astype(F32)
    return high, column - high


def dot(left, right):
    return jnp.dot(left, right, preferred_element_type=F32)


def dot_t(left, right):
    return lax.dot_general(left, right, (((1,), (1,)), ((), ())), preferred_element_type=F32)


def tiles_of(total, step):
    return [(start, min(step, total - start)) for start in range(0, total, step)]


def pieces_of(units):
    blocks = units // LANES
    counts = [share * blocks // sum(SHARES) for share in SHARES]
    counts[0] = blocks - sum(counts[1:])
    head = units - LANES * sum(counts[1:])
    room = (head + 2 + LANES - 1) // LANES * LANES
    pieces, first = [(0, head, room)], head
    for count in counts[1:]:
        pieces.append((first, count * LANES, count * LANES))
        first += count * LANES
    return pieces


def peer_of(me, step, count):
    if count & (count - 1):
        return lax.rem(me + step, count)
    place, bit = 0, 1
    while bit < count:
        own = lax.rem(me // bit, 2)
        place = place + bit * (1 - own if step & bit else own)
        bit *= 2
    return place


def drain(ref, sem):
    pltpu.make_async_copy(ref, ref, sem).wait()


def stacked(array, parts):
    width = array.shape[1] // parts
    return jnp.concatenate([array[:, k * width : (k + 1) * width] for k in range(parts)], axis=0)


def copy_out(*refs):
    *arrays, sems = refs
    half = len(arrays) // 2
    copies = [
        pltpu.make_async_copy(arrays[k], arrays[half + k], sems.at[k]) for k in range(half)
    ]
    for copy in copies:
        copy.start()
    for copy in copies:
        copy.wait()


def layer_kernel(
    n_kv,
    n_tp,
    width,
    tokens_h,
    attn_gain_h,
    wq_h,
    wk_h,
    wv_h,
    wg_h,
    wc_h,
    dw_h,
    db_h,
    head_gain_h,
    key_h,
    value_h,
    decay_h,
    state_h,
    lengths_h,
    wo_h,
    mlp_gain_h,
    gate_h,
    up_h,
    down_h,
    out_ref,
    nk_ref,
    nv_ref,
    tokens,
    attn_gain,
    wq,
    wk,
    wv,
    wg,
    wc,
    dw,
    db,
    head_gain,
    key,
    value,
    decay,
    state,
    lengths_s,
    wo,
    mlp_gain,
    gate,
    up,
    down,
    early,
    early_send,
    early_recv,
    proj,
    proj_send,
    proj_recv,
    keyed,
    keyed_rows,
    value_rows,
    state_rows,
    total_exp,
    keys_send,
    keys_recv,
    values_send,
    values_recv,
    heads_send,
    heads,
    heads_all,
    attended,
    accs,
    sends,
    recvs,
    hiddens,
    hidden_sends,
    hiddens_all,
    lifted,
    load_sem,
    send_sem,
    recv_sem,
):
    kv_me = lax.axis_index("kv")
    tp_me = lax.axis_index("tp")
    tp_mate = tp_me + 1 - 2 * lax.rem(tp_me, 2)
    rows, feats = tokens.shape
    seqs, span, heads_here, key_dim = key.shape
    value_dim = value.shape[3]
    kw, vw = heads_here * key_dim, heads_here * value_dim
    rank = wc.shape[0]
    units = gate.shape[0]
    pieces = pieces_of(units)

    loads = {}
    pairs = [
        ("tokens", tokens_h, tokens),
        ("attn_gain", attn_gain_h, attn_gain),
        ("wc", wc_h, wc),
        ("wq", wq_h, wq),
        ("wk", wk_h, wk),
        ("wv", wv_h, wv),
        ("wg", wg_h, wg),
        ("lengths", lengths_h, lengths_s),
        ("decay", decay_h, decay),
        ("key", key_h, key),
        ("dw", dw_h, dw.at[pl.ds(0, rank)]),
        ("db", db_h, db),
        ("state", state_h, state),
        ("value", value_h, value),
        ("head_gain", head_gain_h, head_gain),
        ("wo", wo_h, wo),
        ("mlp_gain", mlp_gain_h, mlp_gain),
        ("gate", gate_h, gate),
        ("up", up_h, up),
        ("down", down_h, down),
    ]
    given = []
    for place, (name, source, target) in enumerate(pairs):
        if name in SWAPPED_LOADS:
            loads[name] = pltpu.make_async_remote_copy(
                src_ref=source,
                dst_ref=target,
                send_sem=load_sem.at[len(pairs) + len(given)],
                recv_sem=load_sem.at[place],
                device_id={"tp": tp_mate},
                device_id_type=pl.DeviceIdType.MESH,
            )
            given.append(loads[name])
        else:
            loads[name] = pltpu.make_async_copy(source, target, load_sem.at[place])
        if place < FIRST_LOADS:
            loads[name].start()

    def ready(*names):
        for name in names:
            load = loads.pop(name)
            if name in SWAPPED_LOADS:
                load.wait_recv()
            else:
                load.wait()

    barrier = pltpu.get_barrier_semaphore()
    others = [{"kv": peer_of(kv_me, k, n_kv), "tp": tp_mate} for k in range(n_kv)]
    others += [{"tp": lax.rem(tp_mate + 2 * k, n_tp)} for k in range(1, n_tp // 2)]
    others += [{"tp": lax.rem(tp_me + 2 * k, n_tp)} for k in range(1, n_tp // 2)]
    for other in others:
        pl.semaphore_signal(
            barrier, inc=1, device_id=other, device_id_type=pl.DeviceIdType.MESH
        )

    pending = []

    def send(source, target, sem, device):
        pltpu.make_async_remote_copy(
            src_ref=source,
            dst_ref=target,
            send_sem=send_sem.at[sem],
            recv_sem=recv_sem.at[sem],
            device_id=device,
            device_id_type=pl.DeviceIdType.MESH,
        ).start()

    def to_kv(source, target, sem):
        for step in range(n_kv - 1, -1, -1):
            p = peer_of(kv_me, step, n_kv)
            send(source(p), target.at[kv_me], sem, {"kv": p, "tp": tp_mate})
        pending.append((target, sem))

    def to_tp(target, sem):
        for step in range(n_tp - 1, 0, -1):
            p = peer_of(tp_me, step, n_tp)
            send(target.at[tp_me], target.at[tp_me], sem, {"tp": p})
        pending.append((target.at[pl.ds(0, n_tp - 1)], sem))

    def await_tp(target, sem):
        drain(target.at[pl.ds(0, n_tp - 1)], recv_sem.at[sem])

    base_misc = 2 * kw
    ready(*("tokens", "attn_gain", "wc"))
    token_f = tokens[...].astype(F32)
    scaled = (token_f * attn_gain[...]).astype(BF16)
    early[:, base_misc:] = jnp.zeros((rows, LANES), F32)
    early[:, base_misc : base_misc + rank] = dot_t(scaled, wc[...])
    high, low = split_sum(jnp.sum(token_f * token_f, axis=1, keepdims=True))
    early[:, base_misc + rank : base_misc + rank + 1] = high
    early[:, base_misc + rank + 1 : base_misc + rank + 2] = low

    def project(result, base, name, weight):
        ready(name)
        for start, size in tiles_of(weight.shape[1], 256):
            result[:, base + start : base + start + size] = dot(
                scaled, weight[:, start : start + size]
            )

    def scatter(result, outgoing, incoming, sem):
        for p in range(n_kv):
            outgoing[p] = result[p * seqs : (p + 1) * seqs, :].astype(BF16)
        to_kv(lambda p: outgoing.at[p], incoming, sem)

    project(early, 0, "wq", wq)
    project(early, kw, "wk", wk)
    pl.semaphore_wait(barrier, len(others))
    scatter(early, early_send, early_recv, SEM_EARLY)
    loads["lengths"].start()
    for load in given:
        load.start()
    project(proj, 0, "wv", wv)
    project(proj, vw, "wg", wg)
    scatter(proj, proj_send, proj_recv, SEM_PROJ)
    for name, load in loads.items():
        if name not in SWAPPED_LOADS and name != "lengths":
            load.start()

    dw[rank:, :] = jnp.zeros((dw.shape[0] - rank, dw.shape[1]), BF16)
    ready(*("lengths", "decay", "key"))
    positions = lax.broadcasted_iota(jnp.int32, (span, heads_here, key_dim), 0)
    for b in range(seqs):
        live = positions < lengths_s[b]
        kept = jnp.where(live, decay[b], 0.0)
        suffix = kept
        step = 1
        while step < span:
            suffix = suffix + jnp.concatenate(
                [suffix[step:], jnp.zeros((step, heads_here, key_dim), F32)], axis=0
            )
            step *= 2
        for h in range(heads_here):
            total_exp[h * seqs + b : h * seqs + b + 1, :] = jnp.exp(suffix[0, h : h + 1])
        later = jnp.concatenate([suffix[1:], jnp.zeros((1, heads_here, key_dim), F32)], axis=0)
        keyed[b] = jnp.where(live, key[b].astype(F32) * jnp.exp(later), 0.0)
    for b in range(seqs):
        for h in range(heads_here):
            r = h * seqs + b
            keyed_rows[r * span : (r + 1) * span, :] = keyed[b, :, h, :].astype(BF16)
    ready(*("dw", "db", "head_gain", "state", "value"))
    for b in range(seqs):
        block = value[b].astype(F32)
        for h in range(heads_here):
            r = h * seqs + b
            value_rows[r * span : (r + 1) * span, :] = block[:, h, :].astype(BF16)
            state_rows[r * key_dim : (r + 1) * key_dim, :] = state[b, h].astype(BF16)

    def gathered(incoming):
        total = incoming[0].astype(F32)
        for p in range(1, n_kv):
            total = total + incoming[p].astype(F32)
        return total

    drain(early_recv, recv_sem.at[SEM_EARLY])
    total = gathered(early_recv)
    misc = total[:, base_misc:]
    squares = misc[:, rank : rank + 1] + misc[:, rank + 1 : rank + 2]
    inv_rms = lax.rsqrt(squares / width + EPS)
    queries = (total[:, :kw] * inv_rms * key_dim ** (-0.5)).astype(BF16).astype(F32)
    new_keys = (total[:, kw : 2 * kw] * inv_rms).astype(BF16)
    keys_send[...] = new_keys
    send(keys_send, keys_recv, SEM_KEYS, {"tp": tp_mate})
    pending.append((keys_send, SEM_KEYS))
    code = (misc * inv_rms).astype(BF16)
    pre_gate = dot(code, dw[...]) + db[...]
    new_decay = (jnp.minimum(pre_gate, 0.0) - jnp.log1p(jnp.exp(-jnp.abs(pre_gate)))) / GATE_TEMP
    pairs_here = heads_here * seqs
    decayed = stacked(queries * jnp.exp(new_decay), heads_here)
    own = jnp.sum(
        stacked(queries, heads_here) * stacked(new_keys.astype(F32), heads_here),
        axis=-1,
        keepdims=True,
    )

    def own_block(wide):
        each = wide.shape[1] // pairs_here
        pair = lax.broadcasted_iota(jnp.int32, wide.shape, 0)
        place = lax.broadcasted_iota(jnp.int32, wide.shape, 1)
        mine = (place >= pair * each) & (place < (pair + 1) * each)
        return jnp.where(mine, wide, 0.0).astype(BF16)

    into_state = decayed * total_exp[...]
    carried = dot(own_block(jnp.concatenate([into_state] * pairs_here, axis=1)), state_rows[...])
    scores = own_block(dot_t(decayed.astype(BF16), keyed_rows[...]))
    full = carried + dot(scores, value_rows[...])
    drain(proj_recv, recv_sem.at[SEM_PROJ])
    total = gathered(proj_recv)
    new_values = (total[:, :vw] * inv_rms).astype(BF16)
    out_gate = (total[:, vw:] * inv_rms).astype(BF16).astype(F32)
    full = full + own * stacked(new_values.astype(F32), heads_here)
    norm = lax.rsqrt(jnp.mean(full * full, axis=-1, keepdims=True) + EPS)
    g = stacked(out_gate, heads_here)
    mixed = full * norm * head_gain[...] * (g / (1.0 + jnp.exp(-g)))
    for h in range(heads_here):
        heads_send[:, h * value_dim : (h + 1) * value_dim] = mixed[
            h * seqs : (h + 1) * seqs
        ].astype(BF16)
    to_kv(lambda p: heads_send, heads_all, SEM_HEADS)
    values_send[...] = new_values
    send(values_send, values_recv, SEM_VALUES, {"tp": tp_mate})
    pending.append((values_send, SEM_VALUES))
    ready("wo")
    ready("mlp_gain")
    drain(heads_all, recv_sem.at[SEM_HEADS])
    for p in range(n_kv):
        heads[p * seqs : (p + 1) * seqs, :] = heads_all[p].astype(F32)
    attended[tp_me] = dot(heads[...].astype(BF16), wo[...]).astype(BF16)
    to_tp(attended, SEM_ATTEND)
    drain(keys_recv, recv_sem.at[SEM_KEYS])
    drain(values_recv, recv_sem.at[SEM_VALUES])
    for h in range(heads_here):
        keys = keys_recv[:, h * key_dim : (h + 1) * key_dim].astype(F32)
        values = values_recv[:, h * value_dim : (h + 1) * value_dim].astype(F32)
        for b in range(seqs):
            nk_ref[b, h : h + 1, :] = keys[b : b + 1].astype(BF16)
            nv_ref[b, h : h + 1, :] = values[b : b + 1].astype(BF16)
    ready("gate")
    ready("up")
    await_tp(attended, SEM_ATTEND)
    summed = attended[0].astype(F32)
    for p in range(1, n_tp):
        summed = summed + attended[p].astype(F32)
    mid_f = (token_f + summed).astype(BF16).astype(F32)
    scaled_mid = (mid_f * mlp_gain[...]).astype(BF16)

    for part, (first, size, span_cols) in enumerate(pieces):
        mlp_acc = accs[part]
        for base, weight in ((0, gate), (span_cols, up)):
            if size < span_cols:
                mlp_acc[:, base + span_cols - LANES : base + span_cols] = jnp.zeros(
                    (rows, LANES), F32
                )
            for start, count in tiles_of(size, 256):
                mlp_acc[:, base + start : base + start + count] = dot_t(
                    scaled_mid, weight[first + start : first + start + count, :]
                )
        if part == 0:
            high, low = split_sum(jnp.sum(mid_f * mid_f, axis=1, keepdims=True))
            mlp_acc[:, size : size + 1] = high
            mlp_acc[:, size + 1 : size + 2] = low
        scatter(mlp_acc, sends[part], recvs[part], SHARED_SEMS + part)
    for part, (first, size, span_cols) in enumerate(pieces):
        drain(recvs[part], recv_sem.at[SHARED_SEMS + part])
        total = gathered(recvs[part])
        if part == 0:
            squares = total[:, size : size + 1] + total[:, size + 1 : size + 2]
            inv_mid = lax.rsqrt(squares / width + EPS)
        g = total[:, :span_cols] * inv_mid
        mine = g / (1.0 + jnp.exp(-g)) * (total[:, span_cols:] * inv_mid)
        hidden_sends[part][...] = mine.astype(BF16)
        to_kv(
            lambda p, part=part: hidden_sends[part], hiddens_all[part], SHARED_SEMS + PARTS + part
        )
    ready("down")
    acc = jnp.zeros((rows, feats), F32)
    for part, (first, size, span_cols) in enumerate(pieces):
        drain(hiddens_all[part], recv_sem.at[SHARED_SEMS + PARTS + part])
        hidden = hiddens[part]
        for p in range(n_kv):
            hidden[p * seqs : (p + 1) * seqs, :] = hiddens_all[part][p].astype(F32)
        if size < span_cols:
            lane = lax.broadcasted_iota(jnp.int32, (rows, span_cols), 1)
            whole = jnp.where(lane < size, hidden[...], 0.0).astype(BF16)
        else:
            whole = hidden[...].astype(BF16)
        acc = acc + dot(whole, down[first : first + span_cols, :])
    lifted[tp_me] = acc.astype(BF16)
    to_tp(lifted, SEM_LIFT)
    await_tp(lifted, SEM_LIFT)
    summed = lifted[0].astype(F32)
    for p in range(1, n_tp):
        summed = summed + lifted[p].astype(F32)
    out_ref[...] = (mid_f + summed).astype(BF16)
    for load in given:
        load.wait_send()
    for ref, sem in pending:
        drain(ref, send_sem.at[sem])


def on_device(n_kv, n_tp, *args):
    (
        tokens,
        attn_gain,
        wq,
        wk,
        wv,
        wg,
        wc,
        dw,
        db,
        head_gain,
        key,
        value,
        decay,
        state,
        lengths,
        wo,
        mlp_gain,
        gate,
        up,
        down,
    ) = args
    row = lambda a: a.reshape(1, a.shape[0])
    operands = [
        tokens,
        row(attn_gain),
        wq,
        wk,
        wv,
        wg,
        wc.T,
        dw,
        row(db),
        row(head_gain),
        key,
        value,
        decay,
        state,
        lengths,
        wo,
        row(mlp_gain),
        gate.T,
        up.T,
        down,
    ]
    rows, feats = tokens.shape
    seqs, span, heads_here, key_dim = key.shape
    value_dim = value.shape[3]
    kw, vw = heads_here * key_dim, heads_here * value_dim
    pairs = heads_here * seqs
    units = gate.shape[1]
    widths = [piece[2] for piece in pieces_of(units)]
    first_cols = 2 * kw + LANES
    cols = 2 * vw
    vmem = pltpu.VMEM

    def copied(a):
        if a is lengths:
            return pltpu.SMEM(a.shape, a.dtype)
        if a is dw:
            return vmem((LANES, a.shape[1]), a.dtype)
        return vmem(a.shape, a.dtype)

    scratch = [copied(a) for a in operands]
    scratch += [
        vmem((rows, first_cols), F32),
        vmem((n_kv, seqs, first_cols), BF16),
        vmem((n_kv, seqs, first_cols), BF16),
        vmem((rows, cols), F32),
        vmem((n_kv, seqs, cols), BF16),
        vmem((n_kv, seqs, cols), BF16),
        vmem((seqs, span, heads_here, key_dim), F32),
        vmem((pairs * span, key_dim), BF16),
        vmem((pairs * span, value_dim), BF16),
        vmem((pairs * key_dim, value_dim), BF16),
        vmem((pairs, key_dim), F32),
        vmem((seqs, kw), BF16),
        vmem((seqs, kw), BF16),
        vmem((seqs, vw), BF16),
        vmem((seqs, vw), BF16),
        vmem((seqs, vw), BF16),
        vmem((rows, vw), F32),
        vmem((n_kv, seqs, vw), BF16),
        vmem((n_tp, rows, feats), BF16),
        [vmem((rows, 2 * w), F32) for w in widths],
        [vmem((n_kv, seqs, 2 * w), BF16) for w in widths],
        [vmem((n_kv, seqs, 2 * w), BF16) for w in widths],
        [vmem((rows, w), F32) for w in widths],
        [vmem((seqs, w), BF16) for w in widths],
        [vmem((n_kv, seqs, w), BF16) for w in widths],
        vmem((n_tp, rows, feats), BF16),
    ]
    dma = pltpu.SemaphoreType.DMA
    scratch += [dma((len(operands) + len(SWAPPED_LOADS),))]
    scratch += [dma((SHARED_SEMS + 2 * PARTS,))] * 2
    in_specs = [pl.BlockSpec(memory_space=pltpu.HBM)] * len(operands)
    shapes = ((rows, feats), (seqs, heads_here, key_dim), (seqs, heads_here, value_dim))
    results = pl.pallas_call(
        functools.partial(layer_kernel, n_kv, n_tp, feats * n_kv),
        out_shape=tuple(vmem(shape, BF16) for shape in shapes),
        in_specs=in_specs,
        out_specs=(pl.BlockSpec(memory_space=pltpu.VMEM),) * 3,
        scratch_shapes=scratch,
        compiler_params=pltpu.CompilerParams(
            collective_id=0, has_side_effects=True, vmem_limit_bytes=66900000
        ),
        name="layer",
    )(*operands)
    return pl.pallas_call(
        copy_out,
        out_shape=tuple(jax.ShapeDtypeStruct(shape, BF16) for shape in shapes),
        in_specs=(pl.BlockSpec(memory_space=pltpu.VMEM),) * 3,
        out_specs=(pl.BlockSpec(memory_space=pl.ANY),) * 3,
        scratch_shapes=[dma((3,))],
        name="results",
    )(*(pltpu.with_memory_space_constraint(r, pltpu.VMEM) for r in results))


def solution(mesh):
    in_specs = (
        P(None, "kv"),
        P("kv"),
        P("kv", "tp"),
        P("kv", "tp"),
        P("kv", "tp"),
        P("kv", "tp"),
        P("kv", None),
        P(None, "tp"),
        P("tp"),
        P(),
        P("kv", None, "tp", None),
        P("kv", None, "tp", None),
        P("kv", None, "tp", None),
        P("kv", "tp", None, None),
        P("kv"),
        P("tp", "kv"),
        P("kv"),
        P("kv", "tp"),
        P("kv", "tp"),
        P("tp", "kv"),
    )
    out_specs = (P(None, "kv"), P("kv", "tp", None), P("kv", "tp", None))
    return jax.shard_map(
        functools.partial(on_device, mesh.shape["kv"], mesh.shape["tp"]),
        mesh=mesh,
        in_specs=in_specs,
        out_specs=out_specs,
        check_vma=False,
    )
```

```python
import functools

import jax
import jax.numpy as jnp
from jax import lax
from jax.experimental import pallas as pl
from jax.experimental.pallas import tpu as pltpu
from jax.sharding import PartitionSpec as P

EPS = 1e-06
GATE_TEMP = 16.0
FIRST_LOADS = 7
SHARES = (4, 6, 6, 6)
COMPUTE = (0, 1, 2, 3)
PAIRED = (1, 2)
ORDER = (0, 3, 1, 2)
PARTS = len(SHARES)
LANES = 128
SWAPPED_LOADS = ("decay", "key", "dw", "db", "state", "value")
SEM_EARLY, SEM_PROJ, SEM_KEYS, SEM_VALUES = range(4)
SEM_HEADS, SEM_ATTEND, SEM_LIFT, SEM_TAIL = 4, 6, 8, 10
SHARED_SEMS = 11
F32 = jnp.float32
BF16 = jnp.bfloat16


def split_sum(column):
    high = column.astype(BF16).astype(F32)
    return high, column - high


def dot(left, right):
    return jnp.dot(left, right, preferred_element_type=F32)


def dot_t(left, right):
    return lax.dot_general(left, right, (((1,), (1,)), ((), ())), preferred_element_type=F32)


def tiles_of(total, step):
    return [(start, min(step, total - start)) for start in range(0, total, step)]


def pieces_of(units):
    blocks = units // LANES
    counts = [share * blocks // sum(SHARES) for share in SHARES]
    counts[0] = blocks - sum(counts[1:])
    head = units - LANES * sum(counts[1:])
    room = (head + 2 + LANES - 1) // LANES * LANES
    pieces, first = [(0, head, room)], head
    for count in counts[1:]:
        pieces.append((first, count * LANES, count * LANES))
        first += count * LANES
    return pieces


def peer_of(me, step, count):
    place, bit = 0, 1
    while bit < count:
        own = lax.rem(me // bit, 2)
        place = place + bit * (1 - own if step & bit else own)
        bit *= 2
    return place


def slots_of(count):
    return [3 * count // 4 if k in PAIRED else count for k in range(PARTS)]


def drain(ref, sem):
    pltpu.make_async_copy(ref, ref, sem).wait()


def stacked(array, parts):
    width = array.shape[1] // parts
    return jnp.concatenate([array[:, k * width : (k + 1) * width] for k in range(parts)], axis=0)


def copy_out(*refs):
    *arrays, sems = refs
    half = len(arrays) // 2
    copies = [
        pltpu.make_async_copy(arrays[k], arrays[half + k], sems.at[k]) for k in range(half)
    ]
    for copy in copies:
        copy.start()
    for copy in copies:
        copy.wait()


def layer_kernel(
    n_kv,
    n_tp,
    width,
    heads_here,
    tokens_h,
    attn_gain_h,
    wq_h,
    wk_h,
    wv_h,
    wg_h,
    wc_h,
    dw_h,
    db_h,
    head_gain_h,
    key_h,
    value_h,
    decay_h,
    state_h,
    lengths_h,
    wo_h,
    mlp_gain_h,
    gate_h,
    up_h,
    down_h,
    out_ref,
    nk_ref,
    nv_ref,
    tokens,
    attn_gain,
    wq,
    wk,
    wv,
    wg,
    wc,
    dw,
    db,
    head_gain,
    key,
    value,
    decay,
    state,
    lengths_s,
    wo,
    mlp_gain,
    gate,
    up,
    down,
    scaled_mid,
    early,
    early_send,
    early_recv,
    proj,
    proj_send,
    proj_recv,
    keyed_rows,
    value_rows,
    total_exp,
    keys_send,
    keys_recv,
    values_send,
    values_recv,
    heads_send,
    heads_all,
    attended,
    accs,
    sends,
    recvs,
    mate_parts,
    far_sends,
    hidden_sends,
    hiddens_all,
    lifted,
    load_sem,
    send_sem,
    recv_sem,
):
    kv_me = lax.axis_index("kv")
    tp_me = lax.axis_index("tp")
    tp_mate = tp_me + 1 - 2 * lax.rem(tp_me, 2)
    rows, feats = tokens.shape
    seqs, spread, key_dim = key.shape
    value_dim = value.shape[3]
    kw, vw = heads_here * key_dim, heads_here * value_dim
    rank = wc.shape[0]
    units = gate.shape[0]
    pieces = pieces_of(units)
    side, half = lax.rem(kv_me, 2), n_kv // 4
    local = lax.rem(kv_me // 2, half)
    near = kv_me // 2 - local
    far = half - near
    bases, group = (near, far), rows // 2
    slots = (local * 2 + side, 2 * half + local * 2 + side)

    loads = {}
    pairs = [
        ("tokens", tokens_h, tokens),
        ("attn_gain", attn_gain_h, attn_gain),
        ("wc", wc_h, wc),
        ("wq", wq_h, wq),
        ("wk", wk_h, wk),
        ("wv", wv_h, wv),
        ("wg", wg_h, wg),
        ("lengths", lengths_h, lengths_s),
        ("decay", decay_h, decay),
        ("key", key_h, key),
        ("dw", dw_h, dw.at[pl.ds(0, rank)]),
        ("db", db_h, db),
        ("value", value_h, value),
        ("state", state_h, state),
        ("head_gain", head_gain_h, head_gain),
        ("wo", wo_h, wo),
        ("mlp_gain", mlp_gain_h, mlp_gain),
        ("gate", gate_h, gate),
        ("up", up_h, up),
        ("down", down_h, down),
    ]
    given = []
    for place, (name, source, target) in enumerate(pairs):
        if name in SWAPPED_LOADS:
            loads[name] = pltpu.make_async_remote_copy(
                src_ref=source,
                dst_ref=target,
                send_sem=load_sem.at[len(pairs) + len(given)],
                recv_sem=load_sem.at[place],
                device_id={"tp": tp_mate},
                device_id_type=pl.DeviceIdType.MESH,
            )
            given.append(loads[name])
        else:
            loads[name] = pltpu.make_async_copy(source, target, load_sem.at[place])
        if place < FIRST_LOADS:
            loads[name].start()

    def ready(*names):
        for name in names:
            load = loads.pop(name)
            if name in SWAPPED_LOADS:
                load.wait_recv()
            else:
                load.wait()

    barrier = pltpu.get_barrier_semaphore()
    others = [{"kv": peer_of(kv_me, k, n_kv), "tp": tp_mate} for k in range(n_kv)]
    others += [{"tp": lax.rem(tp_mate + 2 * k, n_tp)} for k in range(1, n_tp // 2)]
    others += [{"tp": lax.rem(tp_me + 2 * k, n_tp)} for k in range(1, n_tp // 2)]
    others.append({"kv": kv_me + 1 - 2 * side})
    for other in others:
        pl.semaphore_signal(
            barrier, inc=1, device_id=other, device_id_type=pl.DeviceIdType.MESH
        )

    pending = []

    def send(source, target, sem, device):
        pltpu.make_async_remote_copy(
            src_ref=source,
            dst_ref=target,
            send_sem=send_sem.at[sem],
            recv_sem=recv_sem.at[sem],
            device_id=device,
            device_id_type=pl.DeviceIdType.MESH,
        ).start()

    def to_kv(source, target, near_sem, far_sem):
        for step in range(n_kv - 1, -1, -1):
            p = peer_of(kv_me, step, n_kv)
            distant = step >= n_kv // 2
            send(
                source(p),
                target.at[slots[distant]],
                far_sem if distant else near_sem,
                {"kv": p, "tp": tp_mate},
            )
        if near_sem == far_sem:
            pending.append((target, near_sem))
        else:
            pending.append((target.at[pl.ds(0, 2 * half)], near_sem))
            pending.append((target.at[pl.ds(0, 2 * half)], far_sem))

    def await_kv(target, sem):
        drain(target.at[pl.ds(0, 2 * half)], recv_sem.at[sem])

    def to_tp(target, sem):
        for step in range(n_tp - 1, 0, -1):
            p = peer_of(tp_me, step, n_tp)
            send(target.at[tp_me], target.at[tp_me], sem, {"tp": p})
        pending.append((target.at[pl.ds(0, n_tp - 1)], sem))

    def summed(target, sem):
        drain(target.at[pl.ds(0, n_tp - 1)], recv_sem.at[sem])
        total = target[0].astype(F32)
        for p in range(1, n_tp):
            total = total + target[p].astype(F32)
        return total

    def rows_of(block):
        start = bases[block] * 2 * seqs
        return pl.ds(pl.multiple_of(start, group), group)

    base_misc = 2 * kw
    ready(*("tokens", "attn_gain", "wc"))
    token_f = tokens[...].astype(F32)
    scaled = (token_f * attn_gain[...]).astype(BF16)
    early[:, base_misc:] = jnp.zeros((rows, LANES), F32)
    early[:, base_misc : base_misc + rank] = dot_t(scaled, wc[...])
    high, low = split_sum(jnp.sum(token_f * token_f, axis=1, keepdims=True))
    early[:, base_misc + rank : base_misc + rank + 1] = high
    early[:, base_misc + rank + 1 : base_misc + rank + 2] = low

    def project(result, base, name, weight):
        ready(name)
        for start, size in tiles_of(weight.shape[1], 256):
            result[:, base + start : base + start + size] = dot(
                scaled, weight[:, start : start + size]
            )

    def scatter(result, outgoing, incoming, sem):
        for p in range(n_kv):
            outgoing[p] = result[p * seqs : (p + 1) * seqs, :].astype(BF16)
        to_kv(lambda p: outgoing.at[p], incoming, sem, sem)

    project(early, 0, "wq", wq)
    project(early, kw, "wk", wk)
    pl.semaphore_wait(barrier, len(others))
    scatter(early, early_send, early_recv, SEM_EARLY)
    loads["lengths"].start()
    for load in given:
        load.start()
    project(proj, 0, "wv", wv)
    project(proj, vw, "wg", wg)
    scatter(proj, proj_send, proj_recv, SEM_PROJ)
    for name, load in loads.items():
        if name not in SWAPPED_LOADS and name != "lengths":
            load.start()

    dw[rank:, :] = jnp.zeros((dw.shape[0] - rank, dw.shape[1]), BF16)
    ready(*("lengths", "decay", "key"))
    positions = lax.broadcasted_iota(jnp.int32, (spread, key_dim), 0)
    for b in range(seqs):
        live = positions < lengths_s[b] * heads_here
        kept = jnp.where(live, decay[b], 0.0)
        suffix = kept
        step = heads_here
        while step < spread:
            suffix = suffix + jnp.concatenate(
                [suffix[step:], jnp.zeros((step, key_dim), F32)], axis=0
            )
            step *= 2
        totals = jnp.exp(suffix[:heads_here])
        for h in range(heads_here):
            total_exp[h * seqs + b : h * seqs + b + 1, :] = totals[h : h + 1]
        later = jnp.concatenate(
            [suffix[heads_here:], jnp.zeros((heads_here, key_dim), F32)], axis=0
        )
        keyed_rows[b * spread : (b + 1) * spread, :] = jnp.where(
            live, key[b].astype(F32) * jnp.exp(later), 0.0
        ).astype(BF16)
    ready(*("value", "dw", "db", "head_gain"))
    for b in range(seqs):
        value_rows[b * spread : (b + 1) * spread, :] = value[b].reshape(spread, value_dim)
    pairs_here = heads_here * seqs
    block_shape = (pairs_here, seqs * spread)
    pair = lax.broadcasted_iota(jnp.int32, block_shape, 0)
    place = lax.broadcasted_iota(jnp.int32, block_shape, 1)
    begin = lax.rem(pair, seqs) * spread
    score_mask = (
        (place >= begin)
        & (place < begin + spread)
        & (lax.rem(place, heads_here) == pair // seqs)
    )
    wide_shape = (pairs_here, pairs_here * key_dim)
    pair = lax.broadcasted_iota(jnp.int32, wide_shape, 0)
    place = lax.broadcasted_iota(jnp.int32, wide_shape, 1)
    begin = (lax.rem(pair, seqs) * heads_here + pair // seqs) * key_dim
    state_mask = (place >= begin) & (place < begin + key_dim)

    def gathered(incoming):
        total = incoming[0].astype(F32)
        for p in range(1, incoming.shape[0]):
            total = total + incoming[p].astype(F32)
        return total

    drain(early_recv, recv_sem.at[SEM_EARLY])
    total = gathered(early_recv)
    misc = total[:, base_misc:]
    squares = misc[:, rank : rank + 1] + misc[:, rank + 1 : rank + 2]
    inv_rms = lax.rsqrt(squares / width + EPS)
    queries = (total[:, :kw] * inv_rms * key_dim ** (-0.5)).astype(BF16).astype(F32)
    new_keys = (total[:, kw : 2 * kw] * inv_rms).astype(BF16)
    keys_send[...] = new_keys
    send(keys_send, keys_recv, SEM_KEYS, {"tp": tp_mate})
    pending.append((keys_send, SEM_KEYS))
    code = (misc * inv_rms).astype(BF16)
    pre_gate = dot(code, dw[...]) + db[...]
    new_decay = (jnp.minimum(pre_gate, 0.0) - jnp.log1p(jnp.exp(-jnp.abs(pre_gate)))) / GATE_TEMP
    decayed = stacked(queries * jnp.exp(new_decay), heads_here)
    own = jnp.sum(
        stacked(queries, heads_here) * stacked(new_keys.astype(F32), heads_here),
        axis=-1,
        keepdims=True,
    )
    scores = dot_t(decayed.astype(BF16), keyed_rows[...])
    within = dot(jnp.where(score_mask, scores, 0.0).astype(BF16), value_rows[...])
    into_state = jnp.concatenate([decayed * total_exp[...]] * pairs_here, axis=1)
    ready("state")
    carried = dot(
        jnp.where(state_mask, into_state, 0.0),
        state[...].reshape(pairs_here * key_dim, value_dim),
    )
    full = carried + within
    drain(proj_recv, recv_sem.at[SEM_PROJ])
    total = gathered(proj_recv)
    new_values = (total[:, :vw] * inv_rms).astype(BF16)
    out_gate = (total[:, vw:] * inv_rms).astype(BF16).astype(F32)
    full = full + own * stacked(new_values.astype(F32), heads_here)
    norm = lax.rsqrt(jnp.mean(full * full, axis=-1, keepdims=True) + EPS)
    g = stacked(out_gate, heads_here)
    mixed = full * norm * head_gain[...] * (g / (1.0 + jnp.exp(-g)))
    for h in range(heads_here):
        heads_send[:, h * value_dim : (h + 1) * value_dim] = mixed[
            h * seqs : (h + 1) * seqs
        ].astype(BF16)
    to_kv(lambda p: heads_send, heads_all, SEM_HEADS, SEM_HEADS + 1)
    values_send[...] = new_values
    send(values_send, values_recv, SEM_VALUES, {"tp": tp_mate})
    pending.append((values_send, SEM_VALUES))
    ready("wo")
    ready("mlp_gain")
    for block in range(2):
        await_kv(heads_all, SEM_HEADS + block)
        part = heads_all[pl.ds(2 * half * block, 2 * half)].reshape(group, vw)
        attended[block][tp_me] = dot(part, wo[...]).astype(BF16)
        to_tp(attended[block], SEM_ATTEND + block)
    drain(keys_recv, recv_sem.at[SEM_KEYS])
    drain(values_recv, recv_sem.at[SEM_VALUES])
    for h in range(heads_here):
        keys = keys_recv[:, h * key_dim : (h + 1) * key_dim].astype(F32)
        values = values_recv[:, h * value_dim : (h + 1) * value_dim].astype(F32)
        for b in range(seqs):
            nk_ref[b, h : h + 1, :] = keys[b : b + 1].astype(BF16)
            nv_ref[b, h : h + 1, :] = values[b : b + 1].astype(BF16)
    ready("gate")
    ready("up")
    mids, mid_squares = [], []
    for block in range(2):
        update = summed(attended[block], SEM_ATTEND + block)
        mid_f = (tokens[rows_of(block), :].astype(F32) + update).astype(BF16).astype(F32)
        scaled_mid[block * group : (block + 1) * group, :] = (mid_f * mlp_gain[...]).astype(BF16)
        mids.append(mid_f)
        mid_squares.append(jnp.sum(mid_f * mid_f, axis=1, keepdims=True))

    for part in COMPUTE:
        first, size, span_cols = pieces[part]
        mlp_acc = accs[part]
        for base, weight in ((0, gate), (span_cols, up)):
            if size < span_cols:
                mlp_acc[:, base + span_cols - LANES : base + span_cols] = jnp.zeros(
                    (rows, LANES), F32
                )
            for start, count in tiles_of(size, 256):
                mlp_acc[:, base + start : base + start + count] = dot_t(
                    scaled_mid[...], weight[first + start : first + start + count, :]
                )
        if part == 0:
            high, low = split_sum(jnp.concatenate(mid_squares, axis=0))
            mlp_acc[:, size : size + 1] = high
            mlp_acc[:, size + 1 : size + 2] = low
        for q in range(n_kv):
            line = bases[q // (2 * half)] + q % (2 * half) // 2
            sends[part][q % 2, line] = mlp_acc[q * seqs : (q + 1) * seqs, :].astype(BF16)
        if part not in PAIRED:
            to_kv(
                lambda p, part=part: sends[part].at[lax.rem(p, 2), p // 2],
                recvs[part],
                SHARED_SEMS + part,
                SHARED_SEMS + part,
            )
            continue
        send(
            sends[part].at[1 - side, pl.ds(far, half)],
            mate_parts[part],
            SHARED_SEMS + 2 * PARTS + part,
            {"kv": kv_me + 1 - 2 * side},
        )
        pending.append((mate_parts[part], SHARED_SEMS + 2 * PARTS + part))
        for k in range(half - 1, -1, -1):
            line = near + lax.rem(local + k, half)
            for other in (1 - side, side):
                send(
                    sends[part].at[other, line],
                    recvs[part].at[slots[0]],
                    SHARED_SEMS + part,
                    {"kv": line * 2 + other, "tp": tp_mate},
                )
        pending.append((recvs[part], SHARED_SEMS + part))
    for part in PAIRED:
        drain(mate_parts[part], recv_sem.at[SHARED_SEMS + 2 * PARTS + part])
        for k in range(half):
            both = sends[part][side, far + k].astype(F32) + mate_parts[part][k].astype(F32)
            far_sends[part][k] = both.astype(BF16)
        for k in range(half):
            line = lax.rem(local + k, half)
            send(
                far_sends[part].at[line],
                recvs[part].at[2 * half + local],
                SHARED_SEMS + part,
                {"kv": (far + line) * 2 + side, "tp": tp_mate},
            )
    for part in ORDER:
        first, size, span_cols = pieces[part]
        drain(recvs[part], recv_sem.at[SHARED_SEMS + part])
        total = gathered(recvs[part])
        if part == 0:
            squares = total[:, size : size + 1] + total[:, size + 1 : size + 2]
            inv_mid = lax.rsqrt(squares / width + EPS)
        g = total[:, :span_cols] * inv_mid
        mine = g / (1.0 + jnp.exp(-g)) * (total[:, span_cols:] * inv_mid)
        hidden_sends[part][...] = mine.astype(BF16)
        near_sem = SHARED_SEMS + PARTS + part
        to_kv(
            lambda p, part=part: hidden_sends[part],
            hiddens_all[part],
            near_sem,
            SEM_TAIL if part == ORDER[-1] else near_sem,
        )
    ready("down")
    acc = jnp.zeros((rows, feats), F32)

    def lift(part, blocks):
        first, size, span_cols = pieces[part]
        count = len(blocks) * 2 * half
        hidden = hiddens_all[part][pl.ds(blocks[0] * 2 * half, count)]
        hidden = hidden.reshape(count * seqs, span_cols)
        if size < span_cols:
            lane = lax.broadcasted_iota(jnp.int32, hidden.shape, 1)
            hidden = jnp.where(lane < size, hidden.astype(F32), 0.0).astype(BF16)
        return dot(hidden, down[first : first + span_cols, :])

    acc = jnp.zeros((rows, feats), F32)
    for part in ORDER[:-1]:
        drain(hiddens_all[part], recv_sem.at[SHARED_SEMS + PARTS + part])
        acc = acc + lift(part, (0, 1))
    last = ORDER[-1]
    for block, sem in enumerate((SHARED_SEMS + PARTS + last, SEM_TAIL)):
        await_kv(hiddens_all[last], sem)
        ending = acc[block * group : (block + 1) * group] + lift(last, (block,))
        lifted[block][tp_me] = ending.astype(BF16)
        to_tp(lifted[block], SEM_LIFT + block)
    for block in range(2):
        update = summed(lifted[block], SEM_LIFT + block)
        out_ref[rows_of(block), :] = (mids[block] + update).astype(BF16)
    for load in given:
        load.wait_send()
    for ref, sem in pending:
        drain(ref, send_sem.at[sem])


def on_device(n_kv, n_tp, *args):
    (
        tokens,
        attn_gain,
        wq,
        wk,
        wv,
        wg,
        wc,
        dw,
        db,
        head_gain,
        key,
        value,
        decay,
        state,
        lengths,
        wo,
        mlp_gain,
        gate,
        up,
        down,
    ) = args
    row = lambda a: a.reshape(1, a.shape[0])
    by_position = lambda a: a.reshape(a.shape[0], a.shape[1] * a.shape[2], a.shape[3])
    operands = [
        tokens,
        row(attn_gain),
        wq,
        wk,
        wv,
        wg,
        wc.T,
        dw,
        row(db),
        row(head_gain),
        by_position(key),
        value,
        by_position(decay),
        state,
        lengths,
        wo,
        row(mlp_gain),
        gate.T,
        up.T,
        down,
    ]
    rows, feats = tokens.shape
    seqs, span, heads_here, key_dim = key.shape
    value_dim = value.shape[3]
    kw, vw = heads_here * key_dim, heads_here * value_dim
    pairs = heads_here * seqs
    units = gate.shape[1]
    widths = [piece[2] for piece in pieces_of(units)]
    first_cols = 2 * kw + LANES
    cols = 2 * vw
    vmem = pltpu.VMEM

    def copied(a):
        if a is lengths:
            return pltpu.SMEM(a.shape, a.dtype)
        if a is dw:
            return vmem((LANES, a.shape[1]), a.dtype)
        return vmem(a.shape, a.dtype)

    scratch = [copied(a) for a in operands]
    scratch += [
        vmem((rows, feats), BF16),
        vmem((rows, first_cols), F32),
        vmem((n_kv, seqs, first_cols), BF16),
        vmem((n_kv, seqs, first_cols), BF16),
        vmem((rows, cols), F32),
        vmem((n_kv, seqs, cols), BF16),
        vmem((n_kv, seqs, cols), BF16),
        vmem((pairs * span, key_dim), BF16),
        vmem((pairs * span, value_dim), BF16),
        vmem((pairs, key_dim), F32),
        vmem((seqs, kw), BF16),
        vmem((seqs, kw), BF16),
        vmem((seqs, vw), BF16),
        vmem((seqs, vw), BF16),
        vmem((seqs, vw), BF16),
        vmem((n_kv, seqs, vw), BF16),
        [vmem((n_tp, rows // 2, feats), BF16)] * 2,
        [vmem((rows, 2 * w), F32) for w in widths],
        [vmem((2, n_kv // 2, seqs, 2 * w), BF16) for w in widths],
        [vmem((slots, seqs, 2 * w), BF16) for slots, w in zip(slots_of(n_kv), widths)],
        [vmem((n_kv // 4, seqs, 2 * w), BF16) for w in widths],
        [vmem((n_kv // 4, seqs, 2 * w), BF16) for w in widths],
        [vmem((seqs, w), BF16) for w in widths],
        [vmem((n_kv, seqs, w), BF16) for w in widths],
        [vmem((n_tp, rows // 2, feats), BF16)] * 2,
    ]
    dma = pltpu.SemaphoreType.DMA
    scratch += [dma((len(operands) + len(SWAPPED_LOADS),))]
    scratch += [dma((SHARED_SEMS + 3 * PARTS,))] * 2
    in_specs = [pl.BlockSpec(memory_space=pltpu.HBM)] * len(operands)
    shapes = ((rows, feats), (seqs, heads_here, key_dim), (seqs, heads_here, value_dim))
    results = pl.pallas_call(
        functools.partial(layer_kernel, n_kv, n_tp, feats * n_kv, heads_here),
        out_shape=tuple(vmem(shape, BF16) for shape in shapes),
        in_specs=in_specs,
        out_specs=(pl.BlockSpec(memory_space=pltpu.VMEM),) * 3,
        scratch_shapes=scratch,
        compiler_params=pltpu.CompilerParams(
            collective_id=0, has_side_effects=True, vmem_limit_bytes=66900000
        ),
        name="layer",
    )(*operands)
    return pl.pallas_call(
        copy_out,
        out_shape=tuple(jax.ShapeDtypeStruct(shape, BF16) for shape in shapes),
        in_specs=(pl.BlockSpec(memory_space=pltpu.VMEM),) * 3,
        out_specs=(pl.BlockSpec(memory_space=pl.ANY),) * 3,
        scratch_shapes=[dma((3,))],
        name="results",
    )(*(pltpu.with_memory_space_constraint(r, pltpu.VMEM) for r in results))


def solution(mesh):
    in_specs = (
        P(None, "kv"),
        P("kv"),
        P("kv", "tp"),
        P("kv", "tp"),
        P("kv", "tp"),
        P("kv", "tp"),
        P("kv", None),
        P(None, "tp"),
        P("tp"),
        P(),
        P("kv", None, "tp", None),
        P("kv", None, "tp", None),
        P("kv", None, "tp", None),
        P("kv", "tp", None, None),
        P("kv"),
        P("tp", "kv"),
        P("kv"),
        P("kv", "tp"),
        P("kv", "tp"),
        P("tp", "kv"),
    )
    out_specs = (P(None, "kv"), P("kv", "tp", None), P("kv", "tp", None))
    return jax.shard_map(
        functools.partial(on_device, mesh.shape["kv"], mesh.shape["tp"]),
        mesh=mesh,
        in_specs=in_specs,
        out_specs=out_specs,
        check_vma=False,
    )
```
